32 devices in a mesh: sp: 4 (over z), dp: 8 (over y, x, core).
Axes of the slice: x: 2, y: 2, z: 4, core: 2. Of those that a mesh axis runs over, the one named last changes fastest.
Arguments:
- tokens: bfloat16 [8, 256, 2048], P('dp', 'sp'), may hold values from -6 to 6
- query_weight: bfloat16 [2048, 512], P('dp'), may hold values from -0.125 to 0.125
- key_weight: bfloat16 [2048, 512], P('dp'), may hold values from -0.125 to 0.125
- value_weight: bfloat16 [2048, 1024], P('dp'), may hold values from -0.125 to 0.125
- gate_weight: bfloat16 [2048, 4, 16], P('dp'), may hold values from -0.125 to 0.125
- gate_bias: float32 [4, 16], P(None, 'sp'), may hold values from 2 to 6
- norm_gain: float32 [16, 64], P('sp'), may hold values from 0.5 to 1.5
- out_weight: bfloat16 [1024, 2048], P(None, 'dp'), may hold values from -0.1875 to 0.1875
Outputs:
- mixed: bfloat16 [8, 256, 2048], P('dp', 'sp')
The draws below stay inside these ranges and needn't reach their ends.
All inputs are finite; a program needn't handle non-finite values.
Results may differ from the reference program's by a relative error of at most 0.005.
Values may be sent and summed in bfloat16 or wider, within the bound.
A program may use at most 64 MiB of HBM per device.

```python
import jax
import jax.numpy as jnp
from jax import lax

D = 2048
HEADS = 16
KEY_DIM = 32
VALUE_DIM = 64
BLOCK = 64
SEQ = 256
BATCH = 8


def steps_of(key, shape, cuts, smallest, top_value):
    def one(position, parts):
        steps = jax.random.uniform(jax.random.fold_in(jax.random.fold_in(key, 6), position), (parts,), jnp.float32, smallest / len(cuts), top_value / len(cuts))
        return jnp.repeat(jnp.exp(steps), shape[position] // parts).reshape((-1,) + (1,) * (len(shape) - position - 1))

    factor_of = one(*cuts[0])
    for cut in cuts[1:]:
        factor_of = factor_of * one(*cut)
    return factor_of


def scatter_about(key, extent, scale, bound, shards=(), kind=jnp.bfloat16):
    values = scale * jax.random.normal(key, extent, jnp.float32)
    if shards:
        values = values * steps_of(key, extent, shards, -0.22, 0.18)
    return jnp.clip(values, -bound, bound).astype(kind)


def setup_inputs(seed: int = 0) -> dict:
    key_list = jax.random.split(jax.random.key(seed), 9)
    return {
        "tokens": scatter_about(key_list[0], (BATCH, SEQ, D), 1.0, 6.0, ((0, 8), (1, 4))),
        "query_weight": scatter_about(key_list[1], (D, HEADS * KEY_DIM), D ** -0.5, 0.125, ((0, 8),)),
        "key_weight": scatter_about(key_list[2], (D, HEADS * KEY_DIM), D ** -0.5, 0.125, ((0, 8),)),
        "value_weight": scatter_about(key_list[3], (D, HEADS * VALUE_DIM), D ** -0.5, 0.125, ((0, 8),)),
        "gate_weight": scatter_about(key_list[4], (D, 4, HEADS), D ** -0.5, 0.125, ((0, 8),)),
        "gate_bias": jnp.clip(2.0 + 4.0 * jax.random.uniform(key_list[5], (4, HEADS), jnp.float32) ** steps_of(key_list[5], (4, HEADS), ((1, 4),), -0.2, 0.2), 2.0, 6.0),
        "norm_gain": jnp.clip(1.0 + 0.1 * jax.random.normal(key_list[6], (HEADS, VALUE_DIM), jnp.float32), 0.5, 1.5),
        "out_weight": scatter_about(key_list[7], (HEADS * VALUE_DIM, D), (HEADS * VALUE_DIM) ** -0.5, 0.1875, ((1, 8),)),
    }


norm_eps = 1e-06

def block_scan(queries, key_rows, value_rows, input_gate, log_forget):
    length = queries.shape[0]
    block_count = length // BLOCK
    key_width = queries.shape[1]
    value_width = value_rows.shape[1]
    high = lax.Precision.HIGHEST

    def reshape_blocks(array):
        return array.reshape((block_count, BLOCK) + array.shape[1:])
    causal_mask = jnp.tril(jnp.ones((BLOCK, BLOCK), dtype=bool))

    def advance(carried_state, pieces):
        memory, normal, stabilizer = carried_state
        query_block, key_block, value_block, input_block, forget_block = pieces
        forget_sum = jnp.cumsum(forget_block)
        log_weights = forget_sum[:, None] - forget_sum[None, :] + input_block[None, :]
        log_weights = jnp.where(causal_mask, log_weights, -jnp.inf)
        carry_log = forget_sum + stabilizer
        stab_row = jnp.maximum(carry_log, lax.optimization_barrier(jnp.max(log_weights, axis=1)))
        scores = jnp.dot(query_block, key_block.T, precision=high) * jnp.exp(log_weights - stab_row[:, None])
        carried = jnp.exp(carry_log - stab_row)
        numerator = carried[:, None] * jnp.dot(query_block, memory, precision=high) + jnp.dot(scores, value_block, precision=high)
        denominator = carried * jnp.dot(query_block, normal, precision=high) + lax.optimization_barrier(jnp.sum(scores, axis=1))
        hidden = numerator / jnp.maximum(jnp.abs(denominator), jnp.exp(-stab_row))[:, None]
        forget_total = forget_sum[-1]
        weights_in = forget_total - forget_sum + input_block
        new_stabilizer = jnp.maximum(forget_total + stabilizer, jnp.max(weights_in))
        decay_old = jnp.exp(forget_total + stabilizer - new_stabilizer)
        weights_in = jnp.exp(weights_in - new_stabilizer)
        memory = decay_old * memory + jnp.dot((key_block * weights_in[:, None]).T, value_block, precision=high)
        normal = decay_old * normal + jnp.dot(weights_in, key_block, precision=high)
        return ((memory, normal, new_stabilizer), hidden)
    init_state = (jnp.zeros((key_width, value_width), jnp.float32), jnp.zeros((key_width,), jnp.float32), jnp.zeros((), jnp.float32))
    pieces = (reshape_blocks(queries), reshape_blocks(key_rows), reshape_blocks(value_rows), reshape_blocks(input_gate), reshape_blocks(log_forget))
    final_state, outputs = lax.scan(advance, init_state, pieces)
    return outputs.reshape(length, value_width)

def reverse_time(array):
    return jnp.flip(array, axis=2)

def mix_heads(queries, keys_in, values_in, gate_pre, norm_gain):
    scale_factor = queries.shape[-1] ** (-0.5)
    query_major = jnp.transpose(queries.astype(jnp.float32), (0, 2, 1, 3)) * scale_factor
    key_major = jnp.transpose(keys_in.astype(jnp.float32), (0, 2, 1, 3))
    value_major = jnp.transpose(values_in.astype(jnp.float32), (0, 2, 1, 3))
    gate_major = jnp.transpose(gate_pre, (2, 0, 3, 1))
    input_forward = gate_major[0]
    forget_forward = jax.nn.log_sigmoid(gate_major[1])
    input_backward = gate_major[2]
    forget_backward = jax.nn.log_sigmoid(gate_major[3])
    scan_all = jax.vmap(jax.vmap(block_scan))
    forward = scan_all(query_major, key_major, value_major, input_forward, forget_forward)
    backward = reverse_time(scan_all(reverse_time(query_major), reverse_time(key_major), reverse_time(value_major), reverse_time(input_backward), reverse_time(forget_backward)))
    combined = forward + backward
    normed = combined * lax.rsqrt(lax.optimization_barrier(jnp.mean(combined * combined, axis=-1, keepdims=True)) + norm_eps)
    normed = normed * norm_gain[None, :, None, :]
    return jnp.transpose(normed, (0, 2, 1, 3)).astype(jnp.bfloat16)

def reference(tokens, query_weight, key_weight, value_weight, gate_weight, gate_bias, norm_gain, out_weight):
    batch_count, length, model_width = tokens.shape
    head_count = gate_weight.shape[2]
    flat_tokens = tokens.reshape(batch_count * length, model_width)
    queries = jnp.dot(flat_tokens, query_weight, preferred_element_type=jnp.float32).astype(jnp.bfloat16)
    keys_all = jnp.dot(flat_tokens, key_weight, preferred_element_type=jnp.float32).astype(jnp.bfloat16)
    values_all = jnp.dot(flat_tokens, value_weight, preferred_element_type=jnp.float32).astype(jnp.bfloat16)
    gates = jnp.dot(flat_tokens, gate_weight.reshape(model_width, 4 * head_count), preferred_element_type=jnp.float32)
    query_four = queries.reshape(batch_count, length, head_count, -1)
    key_four = keys_all.reshape(batch_count, length, head_count, -1)
    value_four = values_all.reshape(batch_count, length, head_count, -1)
    gate_four = gates.reshape(batch_count, length, 4, head_count) + gate_bias[None, None]

    def one_sequence(sequence_parts):
        single_query, single_key, single_value, single_gate = sequence_parts
        return mix_heads(single_query[None], single_key[None], single_value[None], single_gate[None], norm_gain)[0]
    normed = lax.map(one_sequence, (query_four, key_four, value_four, gate_four))
    hidden_flat = normed.reshape(batch_count * length, -1)
    output = jnp.dot(hidden_flat, out_weight, preferred_element_type=jnp.float32).astype(jnp.bfloat16)
    return output.reshape(batch_count, length, model_width)
```

```python
import functools

import jax
import jax.numpy as jnp
from jax import lax
from jax.experimental import pallas as pl
from jax.experimental.pallas import tpu as pltpu
from jax.sharding import PartitionSpec as P

BLOCK = 64


norm_eps = 1e-06


def block_scan(queries, key_rows, value_rows, input_gate, log_forget):
    length = queries.shape[0]
    block_count = length // BLOCK
    key_width = queries.shape[1]
    value_width = value_rows.shape[1]
    high = lax.Precision.HIGHEST

    def reshape_blocks(array):
        return array.reshape((block_count, BLOCK) + array.shape[1:])

    causal_mask = jnp.tril(jnp.ones((BLOCK, BLOCK), dtype=bool))

    def advance(carried_state, pieces):
        memory, normal, stabilizer = carried_state
        query_block, key_block, value_block, input_block, forget_block = pieces
        forget_sum = jnp.cumsum(forget_block)
        log_weights = forget_sum[:, None] - forget_sum[None, :] + input_block[None, :]
        log_weights = jnp.where(causal_mask, log_weights, -jnp.inf)
        carry_log = forget_sum + stabilizer
        stab_row = jnp.maximum(carry_log, jnp.max(log_weights, axis=1))
        scores = jnp.dot(query_block, key_block.T, precision=high) * jnp.exp(
            log_weights - stab_row[:, None]
        )
        carried = jnp.exp(carry_log - stab_row)
        numerator = carried[:, None] * jnp.dot(query_block, memory, precision=high) + jnp.dot(
            scores, value_block, precision=high
        )
        denominator = carried * jnp.dot(query_block, normal, precision=high) + jnp.sum(
            scores, axis=1
        )
        hidden = numerator / jnp.maximum(jnp.abs(denominator), jnp.exp(-stab_row))[:, None]
        forget_total = forget_sum[-1]
        weights_in = forget_total - forget_sum + input_block
        new_stabilizer = jnp.maximum(forget_total + stabilizer, jnp.max(weights_in))
        decay_old = jnp.exp(forget_total + stabilizer - new_stabilizer)
        weights_in = jnp.exp(weights_in - new_stabilizer)
        memory = decay_old * memory + jnp.dot(
            (key_block * weights_in[:, None]).T, value_block, precision=high
        )
        normal = decay_old * normal + jnp.dot(weights_in, key_block, precision=high)
        return ((memory, normal, new_stabilizer), hidden)

    init_state = (
        jnp.zeros((key_width, value_width), jnp.float32),
        jnp.zeros((key_width,), jnp.float32),
        jnp.zeros((), jnp.float32),
    )
    pieces = (
        reshape_blocks(queries),
        reshape_blocks(key_rows),
        reshape_blocks(value_rows),
        reshape_blocks(input_gate),
        reshape_blocks(log_forget),
    )
    final_state, outputs = lax.scan(advance, init_state, pieces)
    return outputs.reshape(length, value_width)


def reverse_time(array):
    return jnp.flip(array, axis=2)


def mix_heads(queries, keys_in, values_in, gate_pre, norm_gain):
    scale_factor = queries.shape[-1] ** (-0.5)
    query_major = jnp.transpose(queries.astype(jnp.float32), (0, 2, 1, 3)) * scale_factor
    key_major = jnp.transpose(keys_in.astype(jnp.float32), (0, 2, 1, 3))
    value_major = jnp.transpose(values_in.astype(jnp.float32), (0, 2, 1, 3))
    gate_major = jnp.transpose(gate_pre, (2, 0, 3, 1))
    input_forward = gate_major[0]
    forget_forward = jax.nn.log_sigmoid(gate_major[1])
    input_backward = gate_major[2]
    forget_backward = jax.nn.log_sigmoid(gate_major[3])
    scan_all = jax.vmap(jax.vmap(block_scan))
    forward = scan_all(query_major, key_major, value_major, input_forward, forget_forward)
    backward = reverse_time(
        scan_all(
            reverse_time(query_major),
            reverse_time(key_major),
            reverse_time(value_major),
            reverse_time(input_backward),
            reverse_time(forget_backward),
        )
    )
    combined = forward + backward
    normed = combined * lax.rsqrt(jnp.mean(combined * combined, axis=-1, keepdims=True) + norm_eps)
    normed = normed * norm_gain[None, :, None, :]
    return jnp.transpose(normed, (0, 2, 1, 3)).astype(jnp.bfloat16)


def add_product(partial_value, flat_tokens, weight_rows, offset):
    row_count = weight_rows.shape[0]
    columns = lax.dynamic_slice_in_dim(flat_tokens, offset, row_count, 1)
    return partial_value + jnp.dot(
        columns, weight_rows.reshape(row_count, -1), preferred_element_type=jnp.float32
    )


def local(
    tokens, query_weight, key_weight, value_weight, gate_weight, gate_bias, norm_gain, out_weight
):
    batch_local, token_count, model_width = tokens.shape
    flat_tokens = tokens.reshape(batch_local * token_count, model_width)
    row_total = flat_tokens.shape[0]
    head_count = gate_weight.shape[2]
    key_width = query_weight.shape[1] // head_count
    value_width = value_weight.shape[1] // head_count
    empty_query = jnp.zeros((row_total, query_weight.shape[1]), jnp.float32)
    empty_value = jnp.zeros((row_total, value_weight.shape[1]), jnp.float32)
    empty_gate = jnp.zeros((row_total, 4 * head_count), jnp.float32)

    def fold_one(partial_value, weight_rows, offset):
        return add_product(partial_value, flat_tokens, weight_rows, offset)

    query_raw = fold_one(
        empty_query,
        jax.tree.map(lambda part: lax.all_gather(part, "dp", axis=0, tiled=True), query_weight),
        jnp.int32(0),
    )
    key_raw = fold_one(
        empty_query,
        jax.tree.map(lambda part: lax.all_gather(part, "dp", axis=0, tiled=True), key_weight),
        jnp.int32(0),
    )
    value_raw = fold_one(
        empty_value,
        jax.tree.map(lambda part: lax.all_gather(part, "dp", axis=0, tiled=True), value_weight),
        jnp.int32(0),
    )
    gate_raw = fold_one(
        empty_gate,
        jax.tree.map(lambda part: lax.all_gather(part, "dp", axis=0, tiled=True), gate_weight),
        jnp.int32(0),
    )
    query_local = query_raw.astype(jnp.bfloat16).reshape(
        batch_local, token_count, head_count, key_width
    )
    key_local = key_raw.astype(jnp.bfloat16).reshape(
        batch_local, token_count, head_count, key_width
    )
    value_local = value_raw.astype(jnp.bfloat16).reshape(
        batch_local, token_count, head_count, value_width
    )
    query_local, key_local, value_local = (
        lax.all_to_all(query_local, "sp", split_axis=2, concat_axis=1, tiled=True),
        lax.all_to_all(key_local, "sp", split_axis=2, concat_axis=1, tiled=True),
        lax.all_to_all(value_local, "sp", split_axis=2, concat_axis=1, tiled=True),
    )
    gate_local = gate_raw.reshape(batch_local, token_count, 4, head_count)
    gate_local = (
        lax.all_to_all(gate_local, "sp", split_axis=3, concat_axis=1, tiled=True)
        + gate_bias[None, None]
    )
    normed = mix_heads(query_local, key_local, value_local, gate_local, norm_gain)
    returned = lax.all_to_all(normed, "sp", split_axis=1, concat_axis=2, tiled=True)
    hidden_flat = returned.reshape(row_total, -1)

    def project(weight_cols):
        return jnp.dot(hidden_flat, weight_cols, preferred_element_type=jnp.float32)

    output = project(lax.all_gather(out_weight, "dp", axis=1, tiled=True))
    return output.astype(jnp.bfloat16).reshape(batch_local, token_count, model_width)


MESH = pl.DeviceIdType.MESH
PARTS = 2


def scan_rows(values, combine, identity, backward):
    rows = values.shape[0]
    row_index = lax.broadcasted_iota(jnp.int32, values.shape, 0)
    step = 1
    while step < rows:
        if backward:
            moved = pltpu.roll(values, rows - step, 0)
            moved = jnp.where(row_index < rows - step, moved, identity)
        else:
            moved = pltpu.roll(values, step, 0)
            moved = jnp.where(row_index >= step, moved, identity)
        values = combine(values, moved)
        step *= 2
    return values


def fused_kernel(
    sp,
    head_count,
    tokens_ref,
    query_ref,
    key_ref,
    value_ref,
    gate_ref,
    out_weight_ref,
    bias_ref,
    gain_ref,
    out_ref,
    tok,
    wide,
    gates,
    outw,
    normed_buf,
    hidden,
    local_sem,
    tok_send,
    tok_recv,
    wide_send,
    wide_recv,
    gate_send,
    gate_recv,
    outw_send,
    outw_recv,
    norm_send,
    norm_recv,
):
    s = lax.axis_index("sp")
    d = lax.axis_index("dp")
    core = d % 2
    xpos = (d // 2) % 2
    ypos = d // 4
    mate = d + 1 - 2 * core
    xn = d + 2 - 4 * xpos
    yn = d + 4 - 8 * ypos
    diag = xn + 4 - 8 * ypos
    relay_from = yn + core * (xn - yn)
    relay_to = xn + core * (yn - xn)
    hop = mate - d

    slab = query_ref.shape[0]
    key_cols = query_ref.shape[1] // sp
    value_cols = value_ref.shape[1] // sp
    gate_rows = gate_ref.shape[0]
    block = tokens_ref.shape[0]
    inner = out_weight_ref.shape[0]
    piece = inner // PARTS
    local_heads = head_count // sp
    key_width = key_cols // local_heads
    value_width = value_cols // local_heads
    rows = sp * block

    def wide_slot(index):
        return wide.at[pl.ds(pl.multiple_of(index * slab, slab), slab), :]

    def gate_slot(index):
        return gates.at[pl.ds(pl.multiple_of(index * gate_rows, gate_rows), gate_rows), :]

    def outw_slot(index, part):
        return outw.at[index, pl.ds(part * piece, piece), :]

    def push(ref, send, recv, axis, target):
        return pltpu.make_async_remote_copy(
            src_ref=ref,
            dst_ref=ref,
            send_sem=send,
            recv_sem=recv,
            device_id={axis: target},
            device_id_type=MESH,
        )

    def wide_push(index, number, target):
        return push(wide_slot(index), wide_send.at[number], wide_recv.at[index], "dp", target)

    def gate_push(index, number, target):
        return push(gate_slot(index), gate_send.at[number], gate_recv.at[index], "dp", target)

    def outw_push(index, part, number, target):
        return push(
            outw_slot(index, part),
            outw_send.at[number, part],
            outw_recv.at[index, part],
            "dp",
            target,
        )

    def tok_push(origin, number, target):
        return push(tok.at[origin], tok_send.at[number], tok_recv.at[origin], "sp", target)

    key_at = pl.multiple_of(s * key_cols, key_cols)
    value_at = pl.multiple_of(s * value_cols, value_cols)
    own_rows = pl.ds(pl.multiple_of(d * slab, slab), slab)
    loads = [
        pltpu.make_async_copy(tokens_ref, tok.at[s], local_sem.at[0]),
        pltpu.make_async_copy(
            query_ref.at[:, pl.ds(key_at, key_cols)],
            wide.at[own_rows, pl.ds(0, key_cols)],
            local_sem.at[1],
        ),
        pltpu.make_async_copy(
            key_ref.at[:, pl.ds(key_at, key_cols)],
            wide.at[own_rows, pl.ds(key_cols, key_cols)],
            local_sem.at[2],
        ),
        pltpu.make_async_copy(
            value_ref.at[:, pl.ds(value_at, value_cols)],
            wide.at[own_rows, pl.ds(2 * key_cols, value_cols)],
            local_sem.at[3],
        ),
        pltpu.make_async_copy(gate_ref, gate_slot(d), local_sem.at[4]),
        pltpu.make_async_copy(out_weight_ref, outw.at[d], local_sem.at[5]),
    ]
    for load in loads:
        load.start()

    barrier = pltpu.get_barrier_semaphore()
    for target in (xn, yn, mate):
        pl.semaphore_signal(barrier, inc=1, device_id={"dp": target}, device_id_type=MESH)
    for offset in range(1, sp):
        pl.semaphore_signal(
            barrier, inc=1, device_id={"sp": (s + offset) % sp}, device_id_type=MESH
        )
    pl.semaphore_wait(barrier, 3 + sp - 1)

    def token_stage(k, wait):
        right_origin = s - k
        left_origin = s + k
        has_left = right_origin >= 0
        has_right = left_origin < sp
        if wait:

            @pl.when(has_left)
            def _():
                tok_push(right_origin, 0, s).wait_recv()

        @pl.when(jnp.logical_and(has_left, s + 1 < sp))
        def _():
            tok_push(right_origin, 2 * k, s + 1).start()

        if wait:

            @pl.when(has_right)
            def _():
                tok_push(left_origin, 0, s).wait_recv()

        @pl.when(jnp.logical_and(has_right, s >= 1))
        def _():
            tok_push(left_origin, 2 * k + 1, s - 1).start()

    def token_drain(k):
        @pl.when(jnp.logical_and(s - k >= 0, s + 1 < sp))
        def _():
            tok_push(s - k, 2 * k, s + 1).wait_send()

        @pl.when(jnp.logical_and(s + k < sp, s >= 1))
        def _():
            tok_push(s + k, 2 * k + 1, s - 1).wait_send()

    loads[0].wait()
    token_stage(0, False)
    for load in loads[1:5]:
        load.wait()
    sent = []

    def launch(copy):
        copy.start()
        sent.append(copy)

    for number, target in ((0, xn), (1, yn), (2, mate)):
        launch(wide_push(d, number, target))
        launch(gate_push(d, number, target))
    loads[5].wait()

    def await_wide(index):
        wide_push(index, 0, mate).wait_recv()
        gate_push(index, 0, mate).wait_recv()

    await_wide(relay_from)
    launch(wide_push(relay_from, 3, relay_to))
    launch(gate_push(relay_from, 3, relay_to))
    launch(wide_push(relay_from, 4, mate))
    launch(gate_push(relay_from, 4, mate))
    for part in range(PARTS):
        for number, target in ((0, xn), (1, yn), (2, mate)):
            launch(outw_push(d, part, number, target))
    await_wide(relay_to)
    launch(wide_push(relay_to, 5, mate))
    launch(gate_push(relay_to, 5, mate))
    token_stage(1, True)
    await_wide(diag)
    launch(wide_push(diag, 6, mate))
    launch(gate_push(diag, 6, mate))
    for k in range(2, sp):
        token_stage(k, True)
    for index in (mate, xn + hop, yn + hop, diag + hop):
        await_wide(index)

    flat = tok[...].reshape(rows, tok.shape[2])
    projected = jnp.dot(flat, wide[...], preferred_element_type=jnp.float32).astype(jnp.bfloat16)
    queries = projected[:, :key_cols]
    keys = projected[:, key_cols : 2 * key_cols]
    values = projected[:, 2 * key_cols :]
    slabs = wide.shape[0] // slab
    first = jnp.concatenate(
        [flat[:, i * slab : i * slab + gate_rows] for i in range(slabs)], axis=1
    )
    second = jnp.concatenate(
        [flat[:, i * slab + gate_rows : (i + 1) * slab] for i in range(slabs)], axis=1
    )
    gate_first = jnp.dot(first, gates[...], preferred_element_type=jnp.float32)
    gate_second = jnp.dot(second, gates[...], preferred_element_type=jnp.float32)
    gate_lanes = gate_first.shape[1]
    pre = gate_first + pltpu.roll(gate_second, gate_lanes // 2, 1)
    pre = pltpu.roll(pre, (gate_lanes - s * local_heads) % gate_lanes, 1)

    def outw_relay(part):
        outw_push(relay_from, part, 0, mate).wait_recv()
        launch(outw_push(relay_from, part, 3, relay_to))
        launch(outw_push(relay_from, part, 4, mate))

    for part in range(PARTS - 1):
        outw_relay(part)

    bias_parts = []
    for role in range(4):
        bias_parts.append(bias_ref[role : role + 1, :])
        bias_parts.append(jnp.zeros((1, head_count - local_heads), jnp.float32))
    bias_parts.append(jnp.zeros((1, gate_lanes - 4 * head_count), jnp.float32))
    pre = pre + jnp.concatenate(bias_parts, axis=1)
    log_forget = jnp.minimum(pre, 0.0) - jnp.log1p(jnp.exp(-jnp.abs(pre)))
    lane = lax.broadcasted_iota(jnp.int32, pre.shape, 1)
    is_forward = lane < 2 * head_count
    forget_sum = jnp.where(
        is_forward,
        scan_rows(log_forget, jnp.add, 0.0, False),
        scan_rows(log_forget, jnp.add, 0.0, True),
    )
    forget_sum = pltpu.roll(forget_sum, gate_lanes - head_count, 1)
    source = pre - forget_sum
    peak = jnp.where(
        is_forward,
        scan_rows(source, jnp.maximum, -jnp.inf, False),
        scan_rows(source, jnp.maximum, -jnp.inf, True),
    )
    peak = jnp.maximum(peak, 0.0)
    floor = jnp.exp(-(forget_sum + peak))
    source_rows = jnp.transpose(source)

    row_index = lax.broadcasted_iota(jnp.int32, (rows, rows), 0)
    col_index = lax.broadcasted_iota(jnp.int32, (rows, rows), 1)
    masks = (col_index <= row_index, col_index >= row_index)
    key_lane = lax.broadcasted_iota(jnp.int32, queries.shape, 1) // key_width
    value_lane = lax.broadcasted_iota(jnp.int32, values.shape, 1) // value_width
    scale = key_width ** (-0.5)
    combined = jnp.zeros(values.shape, jnp.float32)
    for h in range(local_heads):
        head_query = jnp.where(key_lane == h, queries, jnp.zeros_like(queries))
        head_value = jnp.where(value_lane == h, values, jnp.zeros_like(values))
        raw = (
            lax.dot_general(
                head_query, keys, (((1,), (1,)), ((), ())), preferred_element_type=jnp.float32
            )
            * scale
        )
        for direction in range(2):
            at = 2 * head_count * direction + h
            exponent = source_rows[at : at + 1, :] - peak[:, at : at + 1]
            weights = raw * jnp.exp(jnp.where(masks[direction], exponent, -jnp.inf))
            total = jnp.sum(weights, axis=1, keepdims=True)
            inverse = 1.0 / jnp.maximum(jnp.abs(total), floor[:, at : at + 1])
            part_sum = jnp.dot(
                weights.astype(jnp.bfloat16), head_value, preferred_element_type=jnp.float32
            )
            combined = combined + part_sum * inverse
    same_head = (
        lax.broadcasted_iota(jnp.int32, (value_cols, value_cols), 0) // value_width
        == lax.broadcasted_iota(jnp.int32, (value_cols, value_cols), 1) // value_width
    )
    mean_square = jnp.dot(
        combined * combined,
        jnp.where(same_head, 1.0 / value_width, 0.0),
        precision=lax.Precision.HIGHEST,
        preferred_element_type=jnp.float32,
    )
    gain = jnp.concatenate([gain_ref[h : h + 1, :] for h in range(local_heads)], axis=1)
    normed = combined * lax.rsqrt(mean_square + norm_eps) * gain
    normed_buf[...] = normed.astype(jnp.bfloat16).reshape(sp, block, value_cols)

    def norm_push(offset):
        target = (s + offset) % sp
        return pltpu.make_async_remote_copy(
            src_ref=normed_buf.at[target],
            dst_ref=hidden.at[s],
            send_sem=norm_send.at[offset - 1],
            recv_sem=norm_recv.at[offset - 1],
            device_id={"sp": target},
            device_id_type=MESH,
        )

    for offset in range(1, sp):
        launch(norm_push(offset))
    outw_relay(PARTS - 1)
    hidden[s] = normed_buf[s]

    for part in range(PARTS):
        outw_push(relay_to, part, 0, mate).wait_recv()
        launch(outw_push(relay_to, part, 5, mate))
    for offset in range(1, sp):
        pltpu.make_async_remote_copy(
            src_ref=normed_buf.at[s],
            dst_ref=hidden.at[(s + sp - offset) % sp],
            send_sem=norm_send.at[offset - 1],
            recv_sem=norm_recv.at[offset - 1],
            device_id={"sp": s},
            device_id_type=MESH,
        ).wait_recv()

    width = outw.shape[2]

    def project(index):
        total = jnp.zeros((block, width), jnp.float32)
        for i in range(sp):
            total = total + jnp.dot(
                hidden[i],
                outw[index, pl.ds(i * value_cols, value_cols), :],
                preferred_element_type=jnp.float32,
            )
        out_ref[:, pl.ds(pl.multiple_of(index * width, width), width)] = total.astype(
            out_ref.dtype
        )

    for index in (d, xn, yn):
        project(index)
    for part in range(PARTS):
        outw_push(diag, part, 0, mate).wait_recv()
        launch(outw_push(diag, part, 6, mate))
    for index in (mate, xn + hop, yn + hop):
        for part in range(PARTS):
            outw_push(index, part, 0, mate).wait_recv()
        project(index)
    project(diag)
    for part in range(PARTS):
        outw_push(diag + hop, part, 0, mate).wait_recv()
    project(diag + hop)
    for copy in sent:
        copy.wait_send()
    for k in range(sp):
        token_drain(k)


def fused_local(
    sp, dp, tokens, query_weight, key_weight, value_weight, gate_weight, gate_bias, norm_gain, out_weight
):
    block, width = tokens.shape[1], tokens.shape[2]
    slab, roles, head_count = gate_weight.shape
    flat_gate = gate_weight.reshape(slab, roles * head_count)
    packed_gate = jnp.concatenate([flat_gate[: slab // 2], flat_gate[slab // 2 :]], axis=1)
    value_cols = value_weight.shape[1] // sp
    wide_cols = (2 * query_weight.shape[1] + value_weight.shape[1]) // sp
    anywhere = pl.BlockSpec(memory_space=pl.ANY)
    vmem = pl.BlockSpec(memory_space=pltpu.VMEM)
    dma = pltpu.SemaphoreType.DMA
    bf16 = jnp.bfloat16
    output = pl.pallas_call(
        functools.partial(fused_kernel, sp, head_count),
        out_shape=jax.ShapeDtypeStruct((block, width), tokens.dtype),
        in_specs=[anywhere] * 6 + [vmem] * 2,
        out_specs=vmem,
        scratch_shapes=[
            pltpu.VMEM((sp, block, width), bf16),
            pltpu.VMEM((dp * slab, wide_cols), bf16),
            pltpu.VMEM((dp * packed_gate.shape[0], packed_gate.shape[1]), bf16),
            pltpu.VMEM((dp,) + out_weight.shape, bf16),
            pltpu.VMEM((sp, block, value_cols), bf16),
            pltpu.VMEM((sp, block, value_cols), bf16),
            dma((6,)),
            dma((2 * sp,)),
            dma((sp,)),
            dma((7,)),
            dma((dp,)),
            dma((7,)),
            dma((dp,)),
            dma((7, PARTS)),
            dma((dp, PARTS)),
            dma((sp - 1,)),
            dma((sp - 1,)),
        ],
        compiler_params=pltpu.CompilerParams(collective_id=0, has_side_effects=True),
    )(
        tokens[0],
        query_weight,
        key_weight,
        value_weight,
        packed_gate,
        out_weight,
        gate_bias,
        norm_gain,
    )
    return output[None]


def choose(
    sp, dp, tokens, query_weight, key_weight, value_weight, gate_weight, gate_bias, norm_gain, out_weight
):
    args = (tokens, query_weight, key_weight, value_weight, gate_weight, gate_bias, norm_gain, out_weight)
    plane_of_four_chips = dp == 2 * 2 * 2
    aligned = (
        tokens.shape[0] == 1
        and query_weight.shape[1] % (128 * sp) == 0
        and value_weight.shape[1] % (128 * sp) == 0
        and gate_weight.shape[1] * gate_weight.shape[2] == 64
    )
    if plane_of_four_chips and aligned:
        return fused_local(sp, dp, *args)
    return local(*args)


def solution(mesh):
    return jax.shard_map(
        functools.partial(choose, mesh.shape["sp"], mesh.shape["dp"]),
        mesh=mesh,
        in_specs=(
            P("dp", "sp", None),
            P("dp", None),
            P("dp", None),
            P("dp", None),
            P("dp", None, None),
            P(None, "sp"),
            P("sp", None),
            P(None, "dp"),
        ),
        out_specs=P("dp", "sp", None),
        check_vma=False,
    )
```

```python
import functools

import jax
import jax.numpy as jnp
from jax import lax
from jax.experimental import pallas as pl
from jax.experimental.pallas import tpu as pltpu
from jax.sharding import PartitionSpec as P

BLOCK = 64


norm_eps = 1e-06


def block_scan(queries, key_rows, value_rows, input_gate, log_forget):
    length = queries.shape[0]
    block_count = length // BLOCK
    key_width = queries.shape[1]
    value_width = value_rows.shape[1]
    high = lax.Precision.HIGHEST

    def reshape_blocks(array):
        return array.reshape((block_count, BLOCK) + array.shape[1:])

    causal_mask = jnp.tril(jnp.ones((BLOCK, BLOCK), dtype=bool))

    def advance(carried_state, pieces):
        memory, normal, stabilizer = carried_state
        query_block, key_block, value_block, input_block, forget_block = pieces
        forget_sum = jnp.cumsum(forget_block)
        log_weights = forget_sum[:, None] - forget_sum[None, :] + input_block[None, :]
        log_weights = jnp.where(causal_mask, log_weights, -jnp.inf)
        carry_log = forget_sum + stabilizer
        stab_row = jnp.maximum(carry_log, jnp.max(log_weights, axis=1))
        scores = jnp.dot(query_block, key_block.T, precision=high) * jnp.exp(
            log_weights - stab_row[:, None]
        )
        carried = jnp.exp(carry_log - stab_row)
        numerator = carried[:, None] * jnp.dot(query_block, memory, precision=high) + jnp.dot(
            scores, value_block, precision=high
        )
        denominator = carried * jnp.dot(query_block, normal, precision=high) + jnp.sum(
            scores, axis=1
        )
        hidden = numerator / jnp.maximum(jnp.abs(denominator), jnp.exp(-stab_row))[:, None]
        forget_total = forget_sum[-1]
        weights_in = forget_total - forget_sum + input_block
        new_stabilizer = jnp.maximum(forget_total + stabilizer, jnp.max(weights_in))
        decay_old = jnp.exp(forget_total + stabilizer - new_stabilizer)
        weights_in = jnp.exp(weights_in - new_stabilizer)
        memory = decay_old * memory + jnp.dot(
            (key_block * weights_in[:, None]).T, value_block, precision=high
        )
        normal = decay_old * normal + jnp.dot(weights_in, key_block, precision=high)
        return ((memory, normal, new_stabilizer), hidden)

    init_state = (
        jnp.zeros((key_width, value_width), jnp.float32),
        jnp.zeros((key_width,), jnp.float32),
        jnp.zeros((), jnp.float32),
    )
    pieces = (
        reshape_blocks(queries),
        reshape_blocks(key_rows),
        reshape_blocks(value_rows),
        reshape_blocks(input_gate),
        reshape_blocks(log_forget),
    )
    final_state, outputs = lax.scan(advance, init_state, pieces)
    return outputs.reshape(length, value_width)


def reverse_time(array):
    return jnp.flip(array, axis=2)


def mix_heads(queries, keys_in, values_in, gate_pre, norm_gain):
    scale_factor = queries.shape[-1] ** (-0.5)
    query_major = jnp.transpose(queries.astype(jnp.float32), (0, 2, 1, 3)) * scale_factor
    key_major = jnp.transpose(keys_in.astype(jnp.float32), (0, 2, 1, 3))
    value_major = jnp.transpose(values_in.astype(jnp.float32), (0, 2, 1, 3))
    gate_major = jnp.transpose(gate_pre, (2, 0, 3, 1))
    input_forward = gate_major[0]
    forget_forward = jax.nn.log_sigmoid(gate_major[1])
    input_backward = gate_major[2]
    forget_backward = jax.nn.log_sigmoid(gate_major[3])
    scan_all = jax.vmap(jax.vmap(block_scan))
    forward = scan_all(query_major, key_major, value_major, input_forward, forget_forward)
    backward = reverse_time(
        scan_all(
            reverse_time(query_major),
            reverse_time(key_major),
            reverse_time(value_major),
            reverse_time(input_backward),
            reverse_time(forget_backward),
        )
    )
    combined = forward + backward
    normed = combined * lax.rsqrt(jnp.mean(combined * combined, axis=-1, keepdims=True) + norm_eps)
    normed = normed * norm_gain[None, :, None, :]
    return jnp.transpose(normed, (0, 2, 1, 3)).astype(jnp.bfloat16)


def add_product(partial_value, flat_tokens, weight_rows, offset):
    row_count = weight_rows.shape[0]
    columns = lax.dynamic_slice_in_dim(flat_tokens, offset, row_count, 1)
    return partial_value + jnp.dot(
        columns, weight_rows.reshape(row_count, -1), preferred_element_type=jnp.float32
    )


def local(
    tokens, query_weight, key_weight, value_weight, gate_weight, gate_bias, norm_gain, out_weight
):
    batch_local, token_count, model_width = tokens.shape
    flat_tokens = tokens.reshape(batch_local * token_count, model_width)
    row_total = flat_tokens.shape[0]
    head_count = gate_weight.shape[2]
    key_width = query_weight.shape[1] // head_count
    value_width = value_weight.shape[1] // head_count
    empty_query = jnp.zeros((row_total, query_weight.shape[1]), jnp.float32)
    empty_value = jnp.zeros((row_total, value_weight.shape[1]), jnp.float32)
    empty_gate = jnp.zeros((row_total, 4 * head_count), jnp.float32)

    def fold_one(partial_value, weight_rows, offset):
        return add_product(partial_value, flat_tokens, weight_rows, offset)

    query_raw = fold_one(
        empty_query,
        jax.tree.map(lambda part: lax.all_gather(part, "dp", axis=0, tiled=True), query_weight),
        jnp.int32(0),
    )
    key_raw = fold_one(
        empty_query,
        jax.tree.map(lambda part: lax.all_gather(part, "dp", axis=0, tiled=True), key_weight),
        jnp.int32(0),
    )
    value_raw = fold_one(
        empty_value,
        jax.tree.map(lambda part: lax.all_gather(part, "dp", axis=0, tiled=True), value_weight),
        jnp.int32(0),
    )
    gate_raw = fold_one(
        empty_gate,
        jax.tree.map(lambda part: lax.all_gather(part, "dp", axis=0, tiled=True), gate_weight),
        jnp.int32(0),
    )
    query_local = query_raw.astype(jnp.bfloat16).reshape(
        batch_local, token_count, head_count, key_width
    )
    key_local = key_raw.astype(jnp.bfloat16).reshape(
        batch_local, token_count, head_count, key_width
    )
    value_local = value_raw.astype(jnp.bfloat16).reshape(
        batch_local, token_count, head_count, value_width
    )
    query_local, key_local, value_local = (
        lax.all_to_all(query_local, "sp", split_axis=2, concat_axis=1, tiled=True),
        lax.all_to_all(key_local, "sp", split_axis=2, concat_axis=1, tiled=True),
        lax.all_to_all(value_local, "sp", split_axis=2, concat_axis=1, tiled=True),
    )
    gate_local = gate_raw.reshape(batch_local, token_count, 4, head_count)
    gate_local = (
        lax.all_to_all(gate_local, "sp", split_axis=3, concat_axis=1, tiled=True)
        + gate_bias[None, None]
    )
    normed = mix_heads(query_local, key_local, value_local, gate_local, norm_gain)
    returned = lax.all_to_all(normed, "sp", split_axis=1, concat_axis=2, tiled=True)
    hidden_flat = returned.reshape(row_total, -1)

    def project(weight_cols):
        return jnp.dot(hidden_flat, weight_cols, preferred_element_type=jnp.float32)

    output = project(lax.all_gather(out_weight, "dp", axis=1, tiled=True))
    return output.astype(jnp.bfloat16).reshape(batch_local, token_count, model_width)


MESH = pl.DeviceIdType.MESH
PARTS = 4


def scan_rows(values, combine, identity, backward):
    rows = values.shape[0]
    row_index = lax.broadcasted_iota(jnp.int32, values.shape, 0)
    step = 1
    while step < rows:
        if backward:
            moved = pltpu.roll(values, rows - step, 0)
            moved = jnp.where(row_index < rows - step, moved, identity)
        else:
            moved = pltpu.roll(values, step, 0)
            moved = jnp.where(row_index >= step, moved, identity)
        values = combine(values, moved)
        step *= 2
    return values


def fused_kernel(
    sp,
    head_count,
    tokens_ref,
    query_ref,
    key_ref,
    value_ref,
    gate_ref,
    out_weight_ref,
    bias_ref,
    gain_ref,
    out_ref,
    tok,
    wide,
    gates,
    outw,
    normed_buf,
    hidden,
    qkv,
    gate_pre,
    local_sem,
    tok_send,
    tok_recv,
    half_recv,
    wide_send,
    wide_recv,
    gate_send,
    gate_recv,
    outw_send,
    outw_recv,
    norm_send,
    norm_recv,
):
    s = lax.axis_index("sp")
    d = lax.axis_index("dp")
    core = d % 2
    xpos = (d // 2) % 2
    ypos = d // 4
    mate = d + 1 - 2 * core
    xn = d + 2 - 4 * xpos
    yn = d + 4 - 8 * ypos
    diag = xn + 4 - 8 * ypos
    relay_from = yn + core * (xn - yn)
    relay_to = xn + core * (yn - xn)
    hop = mate - d

    slab = query_ref.shape[0]
    key_cols = query_ref.shape[1] // sp
    value_cols = value_ref.shape[1] // sp
    roles_heads = gate_ref.shape[0]
    block = tokens_ref.shape[0]
    inner = out_weight_ref.shape[0]
    piece = inner // PARTS
    local_heads = head_count // sp
    key_width = key_cols // local_heads
    value_width = value_cols // local_heads
    rows = sp * block

    def wide_slot(index):
        return wide.at[pl.ds(pl.multiple_of(index * slab, slab), slab), :]

    def gate_slot(index):
        return gates.at[:, pl.ds(pl.multiple_of(index * slab, slab), slab)]

    def outw_slot(index, part):
        return outw.at[index, pl.ds(part * piece, piece), :]

    def push(ref, send, recv, axis, target):
        return pltpu.make_async_remote_copy(
            src_ref=ref,
            dst_ref=ref,
            send_sem=send,
            recv_sem=recv,
            device_id={axis: target},
            device_id_type=MESH,
        )

    def wide_push(index, number, target):
        return push(wide_slot(index), wide_send.at[number], wide_recv.at[index], "dp", target)

    def gate_push(index, number, target):
        return push(gate_slot(index), gate_send.at[number], gate_recv.at[index], "dp", target)

    def outw_push(index, part, number, target):
        return push(
            outw_slot(index, part),
            outw_send.at[number, part],
            outw_recv.at[index, part],
            "dp",
            target,
        )

    def tok_push(origin, number, target):
        return push(tok.at[origin], tok_send.at[number], tok_recv.at[origin], "sp", target)

    key_at = pl.multiple_of(s * key_cols, key_cols)
    value_at = pl.multiple_of(s * value_cols, value_cols)
    own_rows = pl.ds(pl.multiple_of(d * slab, slab), slab)
    loads = [
        pltpu.make_async_copy(tokens_ref, tok.at[s], local_sem.at[0]),
        pltpu.make_async_copy(
            query_ref.at[:, pl.ds(key_at, key_cols)],
            wide.at[own_rows, pl.ds(0, key_cols)],
            local_sem.at[1],
        ),
        pltpu.make_async_copy(
            key_ref.at[:, pl.ds(key_at, key_cols)],
            wide.at[own_rows, pl.ds(key_cols, key_cols)],
            local_sem.at[2],
        ),
        pltpu.make_async_copy(
            value_ref.at[:, pl.ds(value_at, value_cols)],
            wide.at[own_rows, pl.ds(2 * key_cols, value_cols)],
            local_sem.at[3],
        ),
        pltpu.make_async_copy(gate_ref, gate_slot(d), local_sem.at[4]),
        pltpu.make_async_copy(out_weight_ref, outw.at[d], local_sem.at[5]),
    ]
    for load in loads:
        load.start()

    barrier = pltpu.get_barrier_semaphore()
    for target in (xn, yn, mate):
        pl.semaphore_signal(barrier, inc=1, device_id={"dp": target}, device_id_type=MESH)
    for offset in range(1, sp):
        pl.semaphore_signal(
            barrier, inc=1, device_id={"sp": (s + offset) % sp}, device_id_type=MESH
        )
    pl.semaphore_wait(barrier, 3 + sp - 1)

    right = (s + 1) % sp
    left = (s + sp - 1) % sp
    half = block // 2

    def tok_half(origin, number, part, target):
        ref = tok.at[origin, pl.ds(part * half, half), :]
        return push(ref, tok_send.at[number], half_recv.at[part], "sp", target)

    def token_stage(k, wait):
        if k == 0:
            tok_push(s, 0, right).start()
            tok_push(s, 1, left).start()
        if k == 1:
            tok_push(left, 0, s).wait_recv()
            tok_half(left, 2, 0, right).start()
            tok_push(right, 0, s).wait_recv()
            tok_half(right, 3, 1, left).start()
        if k == 2:
            far = (s + 2) % sp
            tok_half(far, 2, 0, s).wait_recv()
            tok_half(far, 3, 1, s).wait_recv()

    def token_drain(k):
        if k == 0:
            tok_push(s, 0, right).wait_send()
            tok_push(s, 1, left).wait_send()
        if k == 1:
            tok_half(left, 2, 0, right).wait_send()
            tok_half(right, 3, 1, left).wait_send()

    loads[0].wait()
    token_stage(0, False)
    for load in loads[1:5]:
        load.wait()
    sent = []

    def launch(copy):
        copy.start()
        sent.append(copy)

    for number, target in ((0, relay_from), (1, relay_to), (2, mate)):
        launch(wide_push(d, number, target))
        launch(gate_push(d, number, target))
    loads[5].wait()
    for part in range(PARTS):
        launch(outw_push(d, part, 0, relay_from))
        launch(outw_push(d, part, 2, mate))

    def await_wide(index):
        wide_push(index, 0, mate).wait_recv()
        gate_push(index, 0, mate).wait_recv()

    def await_outw(index, part):
        outw_push(index, part, 0, mate).wait_recv()

    await_wide(relay_from)
    launch(wide_push(relay_from, 3, relay_to))
    launch(gate_push(relay_from, 3, relay_to))
    launch(wide_push(relay_from, 4, mate))
    launch(gate_push(relay_from, 4, mate))
    for part in range(PARTS):
        launch(outw_push(d, part, 1, relay_to))
    await_wide(relay_to)
    launch(wide_push(relay_to, 5, mate))
    launch(gate_push(relay_to, 5, mate))
    token_stage(1, True)
    await_wide(diag)
    launch(wide_push(diag, 6, mate))
    launch(gate_push(diag, 6, mate))
    for index in (mate, xn + hop, yn + hop, diag + hop):
        await_wide(index)

    gate_lanes = 2 * roles_heads

    def project_block(index):
        flat = tok[index]
        qkv[index] = jnp.dot(flat, wide[...], preferred_element_type=jnp.float32).astype(
            jnp.bfloat16
        )
        gate_pre[index, :, :roles_heads] = lax.dot_general(
            flat, gates[...], (((1,), (1,)), ((), ())), preferred_element_type=jnp.float32
        )

    gate_pre[...] = jnp.zeros_like(gate_pre)
    for index in (s, left, right):
        project_block(index)
    for part in range(PARTS):
        await_outw(relay_from, part)
        launch(outw_push(relay_from, part, 3, relay_to))
        launch(outw_push(relay_from, part, 4, mate))
    token_stage(2, True)
    project_block((s + 2) % sp)
    projected = qkv[...].reshape(rows, qkv.shape[2])
    queries = projected[:, :key_cols]
    keys = projected[:, key_cols : 2 * key_cols]
    values = projected[:, 2 * key_cols :]
    pre = gate_pre[...].reshape(rows, gate_lanes)
    pre = pltpu.roll(pre, (gate_lanes - s * local_heads) % gate_lanes, 1)

    bias_parts = []
    for role in range(4):
        bias_parts.append(bias_ref[role : role + 1, :])
        bias_parts.append(jnp.zeros((1, head_count - local_heads), jnp.float32))
    bias_parts.append(jnp.zeros((1, gate_lanes - 4 * head_count), jnp.float32))
    pre = pre + jnp.concatenate(bias_parts, axis=1)
    log_forget = jnp.minimum(pre, 0.0) - jnp.log1p(jnp.exp(-jnp.abs(pre)))
    lane = lax.broadcasted_iota(jnp.int32, pre.shape, 1)
    is_forward = lane < 2 * head_count
    forget_sum = jnp.where(
        is_forward,
        scan_rows(log_forget, jnp.add, 0.0, False),
        scan_rows(log_forget, jnp.add, 0.0, True),
    )
    forget_sum = pltpu.roll(forget_sum, gate_lanes - head_count, 1)
    source = pre - forget_sum
    peak = jnp.where(
        is_forward,
        scan_rows(source, jnp.maximum, -jnp.inf, False),
        scan_rows(source, jnp.maximum, -jnp.inf, True),
    )
    peak = jnp.maximum(peak, 0.0)
    floor = jnp.exp(-(forget_sum + peak))
    source_rows = jnp.transpose(source)

    row_index = lax.broadcasted_iota(jnp.int32, (rows, rows), 0)
    col_index = lax.broadcasted_iota(jnp.int32, (rows, rows), 1)
    masks = (col_index <= row_index, col_index >= row_index)
    key_lane = lax.broadcasted_iota(jnp.int32, queries.shape, 1) // key_width
    value_lane = lax.broadcasted_iota(jnp.int32, values.shape, 1) // value_width
    scale = key_width ** (-0.5)
    combined = jnp.zeros(values.shape, jnp.float32)
    for h in range(local_heads):
        head_query = jnp.where(key_lane == h, queries, jnp.zeros_like(queries))
        head_value = jnp.where(value_lane == h, values, jnp.zeros_like(values))
        raw = lax.dot_general(
            head_query, keys, (((1,), (1,)), ((), ())), preferred_element_type=jnp.float32
        )
        for direction in range(2):
            at = 2 * head_count * direction + h
            exponent = source_rows[at : at + 1, :] - peak[:, at : at + 1]
            weights = raw * jnp.exp(jnp.where(masks[direction], exponent, -jnp.inf))
            total = jnp.sum(weights, axis=1, keepdims=True) * scale
            inverse = scale / jnp.maximum(jnp.abs(total), floor[:, at : at + 1])
            part_sum = jnp.dot(
                weights.astype(jnp.bfloat16), head_value, preferred_element_type=jnp.float32
            )
            combined = combined + part_sum * inverse
    same_head = (
        lax.broadcasted_iota(jnp.int32, (value_cols, value_cols), 0) // value_width
        == lax.broadcasted_iota(jnp.int32, (value_cols, value_cols), 1) // value_width
    )
    ones = jnp.where(same_head, 1.0, 0.0).astype(jnp.bfloat16)
    square = combined * combined
    square_high = square.astype(jnp.bfloat16)
    square_low = (square - square_high.astype(jnp.float32)).astype(jnp.bfloat16)
    mean_square = (
        jnp.dot(square_high, ones, preferred_element_type=jnp.float32)
        + jnp.dot(square_low, ones, preferred_element_type=jnp.float32)
    ) * (1.0 / value_width)
    gain = jnp.concatenate([gain_ref[h : h + 1, :] for h in range(local_heads)], axis=1)
    normed = combined * lax.rsqrt(mean_square + norm_eps) * gain
    normed_buf[...] = normed.astype(jnp.bfloat16).reshape(sp, block, value_cols)

    def norm_push(offset):
        target = (s + offset) % sp
        return pltpu.make_async_remote_copy(
            src_ref=normed_buf.at[target],
            dst_ref=hidden.at[s],
            send_sem=norm_send.at[offset - 1],
            recv_sem=norm_recv.at[offset - 1],
            device_id={"sp": target},
            device_id_type=MESH,
        )

    for offset in range(1, sp):
        launch(norm_push(offset))
    hidden[s] = normed_buf[s]

    for part in range(PARTS):
        await_outw(relay_to, part)
        launch(outw_push(relay_to, part, 5, mate))
    for offset in range(1, sp):
        pltpu.make_async_remote_copy(
            src_ref=normed_buf.at[s],
            dst_ref=hidden.at[(s + sp - offset) % sp],
            send_sem=norm_send.at[offset - 1],
            recv_sem=norm_recv.at[offset - 1],
            device_id={"sp": s},
            device_id_type=MESH,
        ).wait_recv()

    width = outw.shape[2]

    def project(index):
        total = jnp.zeros((block, width), jnp.float32)
        for i in range(sp):
            total = total + jnp.dot(
                hidden[i],
                outw[index, pl.ds(i * value_cols, value_cols), :],
                preferred_element_type=jnp.float32,
            )
        out_ref[:, pl.ds(pl.multiple_of(index * width, width), width)] = total.astype(
            out_ref.dtype
        )

    for index in (d, xn, yn):
        project(index)
    for part in range(PARTS):
        outw_push(diag, part, 0, mate).wait_recv()
        launch(outw_push(diag, part, 6, mate))
    for index in (mate, xn + hop, yn + hop):
        for part in range(PARTS):
            outw_push(index, part, 0, mate).wait_recv()
        project(index)
    project(diag)
    for part in range(PARTS):
        outw_push(diag + hop, part, 0, mate).wait_recv()
    project(diag + hop)
    for copy in sent:
        copy.wait_send()
    for k in range(sp):
        token_drain(k)


def fused_local(
    sp, dp, tokens, query_weight, key_weight, value_weight, gate_weight, gate_bias, norm_gain, out_weight
):
    block, width = tokens.shape[1], tokens.shape[2]
    slab, roles, head_count = gate_weight.shape
    gate_rows = jnp.transpose(gate_weight, (1, 2, 0)).reshape(roles * head_count, slab)
    value_cols = value_weight.shape[1] // sp
    wide_cols = (2 * query_weight.shape[1] + value_weight.shape[1]) // sp
    anywhere = pl.BlockSpec(memory_space=pl.ANY)
    vmem = pl.BlockSpec(memory_space=pltpu.VMEM)
    dma = pltpu.SemaphoreType.DMA
    bf16 = jnp.bfloat16
    output = pl.pallas_call(
        functools.partial(fused_kernel, sp, head_count),
        out_shape=jax.ShapeDtypeStruct((block, width), tokens.dtype),
        in_specs=[anywhere] * 6 + [vmem] * 2,
        out_specs=vmem,
        scratch_shapes=[
            pltpu.VMEM((sp, block, width), bf16),
            pltpu.VMEM((dp * slab, wide_cols), bf16),
            pltpu.VMEM((roles * head_count, dp * slab), bf16),
            pltpu.VMEM((dp,) + out_weight.shape, bf16),
            pltpu.VMEM((sp, block, value_cols), bf16),
            pltpu.VMEM((sp, block, value_cols), bf16),
            pltpu.VMEM((sp, block, wide_cols), bf16),
            pltpu.VMEM((sp, block, 2 * roles * head_count), jnp.float32),
            dma((6,)),
            dma((2 * sp,)),
            dma((sp,)),
            dma((2,)),
            dma((7,)),
            dma((dp,)),
            dma((7,)),
            dma((dp,)),
            dma((7, PARTS)),
            dma((dp, PARTS)),
            dma((sp - 1,)),
            dma((sp - 1,)),
        ],
        compiler_params=pltpu.CompilerParams(collective_id=0, has_side_effects=True),
    )(
        tokens[0],
        query_weight,
        key_weight,
        value_weight,
        gate_rows,
        out_weight,
        gate_bias,
        norm_gain,
    )
    return output[None]


def choose(
    sp, dp, tokens, query_weight, key_weight, value_weight, gate_weight, gate_bias, norm_gain, out_weight
):
    args = (tokens, query_weight, key_weight, value_weight, gate_weight, gate_bias, norm_gain, out_weight)
    plane_of_four_chips = dp == 2 * 2 * 2
    aligned = (
        tokens.shape[0] == 1
        and query_weight.shape[1] % (128 * sp) == 0
        and value_weight.shape[1] % (128 * sp) == 0
        and gate_weight.shape[1] * gate_weight.shape[2] == 64
    )
    if plane_of_four_chips and sp == 2 + 2 and aligned:
        return fused_local(sp, dp, *args)
    return local(*args)


def solution(mesh):
    return jax.shard_map(
        functools.partial(choose, mesh.shape["sp"], mesh.shape["dp"]),
        mesh=mesh,
        in_specs=(
            P("dp", "sp", None),
            P("dp", None),
            P("dp", None),
            P("dp", None),
            P("dp", None, None),
            P(None, "sp"),
            P("sp", None),
            P(None, "dp"),
        ),
        out_specs=P("dp", "sp", None),
        check_vma=False,
    )
```

```python
import functools

import jax
import jax.numpy as jnp
from jax import lax
from jax.experimental import pallas as pl
from jax.experimental.pallas import tpu as pltpu
from jax.sharding import PartitionSpec as P

BLOCK = 64


norm_eps = 1e-06


def block_scan(queries, key_rows, value_rows, input_gate, log_forget):
    length = queries.shape[0]
    block_count = length // BLOCK
    key_width = queries.shape[1]
    value_width = value_rows.shape[1]
    high = lax.Precision.HIGHEST

    def reshape_blocks(array):
        return array.reshape((block_count, BLOCK) + array.shape[1:])

    causal_mask = jnp.tril(jnp.ones((BLOCK, BLOCK), dtype=bool))

    def advance(carried_state, pieces):
        memory, normal, stabilizer = carried_state
        query_block, key_block, value_block, input_block, forget_block = pieces
        forget_sum = jnp.cumsum(forget_block)
        log_weights = forget_sum[:, None] - forget_sum[None, :] + input_block[None, :]
        log_weights = jnp.where(causal_mask, log_weights, -jnp.inf)
        carry_log = forget_sum + stabilizer
        stab_row = jnp.maximum(carry_log, jnp.max(log_weights, axis=1))
        scores = jnp.dot(query_block, key_block.T, precision=high) * jnp.exp(
            log_weights - stab_row[:, None]
        )
        carried = jnp.exp(carry_log - stab_row)
        numerator = carried[:, None] * jnp.dot(query_block, memory, precision=high) + jnp.dot(
            scores, value_block, precision=high
        )
        denominator = carried * jnp.dot(query_block, normal, precision=high) + jnp.sum(
            scores, axis=1
        )
        hidden = numerator / jnp.maximum(jnp.abs(denominator), jnp.exp(-stab_row))[:, None]
        forget_total = forget_sum[-1]
        weights_in = forget_total - forget_sum + input_block
        new_stabilizer = jnp.maximum(forget_total + stabilizer, jnp.max(weights_in))
        decay_old = jnp.exp(forget_total + stabilizer - new_stabilizer)
        weights_in = jnp.exp(weights_in - new_stabilizer)
        memory = decay_old * memory + jnp.dot(
            (key_block * weights_in[:, None]).T, value_block, precision=high
        )
        normal = decay_old * normal + jnp.dot(weights_in, key_block, precision=high)
        return ((memory, normal, new_stabilizer), hidden)

    init_state = (
        jnp.zeros((key_width, value_width), jnp.float32),
        jnp.zeros((key_width,), jnp.float32),
        jnp.zeros((), jnp.float32),
    )
    pieces = (
        reshape_blocks(queries),
        reshape_blocks(key_rows),
        reshape_blocks(value_rows),
        reshape_blocks(input_gate),
        reshape_blocks(log_forget),
    )
    final_state, outputs = lax.scan(advance, init_state, pieces)
    return outputs.reshape(length, value_width)


def reverse_time(array):
    return jnp.flip(array, axis=2)


def mix_heads(queries, keys_in, values_in, gate_pre, norm_gain):
    scale_factor = queries.shape[-1] ** (-0.5)
    query_major = jnp.transpose(queries.astype(jnp.float32), (0, 2, 1, 3)) * scale_factor
    key_major = jnp.transpose(keys_in.astype(jnp.float32), (0, 2, 1, 3))
    value_major = jnp.transpose(values_in.astype(jnp.float32), (0, 2, 1, 3))
    gate_major = jnp.transpose(gate_pre, (2, 0, 3, 1))
    input_forward = gate_major[0]
    forget_forward = jax.nn.log_sigmoid(gate_major[1])
    input_backward = gate_major[2]
    forget_backward = jax.nn.log_sigmoid(gate_major[3])
    scan_all = jax.vmap(jax.vmap(block_scan))
    forward = scan_all(query_major, key_major, value_major, input_forward, forget_forward)
    backward = reverse_time(
        scan_all(
            reverse_time(query_major),
            reverse_time(key_major),
            reverse_time(value_major),
            reverse_time(input_backward),
            reverse_time(forget_backward),
        )
    )
    combined = forward + backward
    normed = combined * lax.rsqrt(jnp.mean(combined * combined, axis=-1, keepdims=True) + norm_eps)
    normed = normed * norm_gain[None, :, None, :]
    return jnp.transpose(normed, (0, 2, 1, 3)).astype(jnp.bfloat16)


def add_product(partial_value, flat_tokens, weight_rows, offset):
    row_count = weight_rows.shape[0]
    columns = lax.dynamic_slice_in_dim(flat_tokens, offset, row_count, 1)
    return partial_value + jnp.dot(
        columns, weight_rows.reshape(row_count, -1), preferred_element_type=jnp.float32
    )


def local(
    tokens, query_weight, key_weight, value_weight, gate_weight, gate_bias, norm_gain, out_weight
):
    batch_local, token_count, model_width = tokens.shape
    flat_tokens = tokens.reshape(batch_local * token_count, model_width)
    row_total = flat_tokens.shape[0]
    head_count = gate_weight.shape[2]
    key_width = query_weight.shape[1] // head_count
    value_width = value_weight.shape[1] // head_count
    empty_query = jnp.zeros((row_total, query_weight.shape[1]), jnp.float32)
    empty_value = jnp.zeros((row_total, value_weight.shape[1]), jnp.float32)
    empty_gate = jnp.zeros((row_total, 4 * head_count), jnp.float32)

    def fold_one(partial_value, weight_rows, offset):
        return add_product(partial_value, flat_tokens, weight_rows, offset)

    query_raw = fold_one(
        empty_query,
        jax.tree.map(lambda part: lax.all_gather(part, "dp", axis=0, tiled=True), query_weight),
        jnp.int32(0),
    )
    key_raw = fold_one(
        empty_query,
        jax.tree.map(lambda part: lax.all_gather(part, "dp", axis=0, tiled=True), key_weight),
        jnp.int32(0),
    )
    value_raw = fold_one(
        empty_value,
        jax.tree.map(lambda part: lax.all_gather(part, "dp", axis=0, tiled=True), value_weight),
        jnp.int32(0),
    )
    gate_raw = fold_one(
        empty_gate,
        jax.tree.map(lambda part: lax.all_gather(part, "dp", axis=0, tiled=True), gate_weight),
        jnp.int32(0),
    )
    query_local = query_raw.astype(jnp.bfloat16).reshape(
        batch_local, token_count, head_count, key_width
    )
    key_local = key_raw.astype(jnp.bfloat16).reshape(
        batch_local, token_count, head_count, key_width
    )
    value_local = value_raw.astype(jnp.bfloat16).reshape(
        batch_local, token_count, head_count, value_width
    )
    query_local, key_local, value_local = (
        lax.all_to_all(query_local, "sp", split_axis=2, concat_axis=1, tiled=True),
        lax.all_to_all(key_local, "sp", split_axis=2, concat_axis=1, tiled=True),
        lax.all_to_all(value_local, "sp", split_axis=2, concat_axis=1, tiled=True),
    )
    gate_local = gate_raw.reshape(batch_local, token_count, 4, head_count)
    gate_local = (
        lax.all_to_all(gate_local, "sp", split_axis=3, concat_axis=1, tiled=True)
        + gate_bias[None, None]
    )
    normed = mix_heads(query_local, key_local, value_local, gate_local, norm_gain)
    returned = lax.all_to_all(normed, "sp", split_axis=1, concat_axis=2, tiled=True)
    hidden_flat = returned.reshape(row_total, -1)

    def project(weight_cols):
        return jnp.dot(hidden_flat, weight_cols, preferred_element_type=jnp.float32)

    output = project(lax.all_gather(out_weight, "dp", axis=1, tiled=True))
    return output.astype(jnp.bfloat16).reshape(batch_local, token_count, model_width)


MESH = pl.DeviceIdType.MESH
PARTS = 4


def scan_rows(values, combine, identity, backward):
    rows = values.shape[0]
    row_index = lax.broadcasted_iota(jnp.int32, values.shape, 0)
    step = 1
    while step < rows:
        if backward:
            moved = pltpu.roll(values, rows - step, 0)
            moved = jnp.where(row_index < rows - step, moved, identity)
        else:
            moved = pltpu.roll(values, step, 0)
            moved = jnp.where(row_index >= step, moved, identity)
        values = combine(values, moved)
        step *= 2
    return values


def fused_kernel(
    sp,
    head_count,
    tokens_ref,
    query_ref,
    key_ref,
    value_ref,
    gate_ref,
    out_weight_ref,
    bias_ref,
    gain_ref,
    out_ref,
    tok,
    wide,
    gates,
    gate_all,
    outw,
    normed_buf,
    hidden,
    qkv,
    total_out,
    gate_pre,
    local_sem,
    tok_send,
    tok_recv,
    half_recv,
    wide_send,
    wide_recv,
    gate_send,
    gate_recv,
    outw_send,
    outw_recv,
    norm_send,
    norm_recv,
):
    s = lax.axis_index("sp")
    d = lax.axis_index("dp")
    core = d % 2
    xpos = (d // 2) % 2
    ypos = d // 4
    mate = d + 1 - 2 * core
    xn = d + 2 - 4 * xpos
    yn = d + 4 - 8 * ypos
    diag = xn + 4 - 8 * ypos
    relay_from = yn + core * (xn - yn)
    relay_to = xn + core * (yn - xn)
    hop = mate - d

    slab = query_ref.shape[0]
    key_cols = query_ref.shape[1] // sp
    value_cols = value_ref.shape[1] // sp
    roles_heads = gate_ref.shape[0]
    block = tokens_ref.shape[0]
    inner = out_weight_ref.shape[0]
    piece = inner // PARTS
    local_heads = head_count // sp
    key_width = key_cols // local_heads
    value_width = value_cols // local_heads
    rows = sp * block

    def wide_slot(index):
        return wide.at[pl.ds(pl.multiple_of(index * slab, slab), slab), :]

    def gate_slot(index):
        return gates.at[:, pl.ds(pl.multiple_of(index * slab, slab), slab)]

    def outw_slot(index, part):
        return outw.at[index, pl.ds(part * piece, piece), :]

    def push(ref, send, recv, axis, target):
        return pltpu.make_async_remote_copy(
            src_ref=ref,
            dst_ref=ref,
            send_sem=send,
            recv_sem=recv,
            device_id={axis: target},
            device_id_type=MESH,
        )

    def wide_push(index, number, target):
        return push(wide_slot(index), wide_send.at[number], wide_recv.at[index], "dp", target)

    def gate_push(index, number, target):
        return push(gate_slot(index), gate_send.at[number], gate_recv.at[index], "dp", target)

    def outw_push(index, part, number, target):
        return push(
            outw_slot(index, part),
            outw_send.at[number, part],
            outw_recv.at[index, part],
            "dp",
            target,
        )

    def tok_push(origin, number, target):
        return push(tok.at[origin], tok_send.at[number], tok_recv.at[origin], "sp", target)

    key_at = pl.multiple_of(s * key_cols, key_cols)
    value_at = pl.multiple_of(s * value_cols, value_cols)
    own_rows = pl.ds(pl.multiple_of(d * slab, slab), slab)
    loads = [
        pltpu.make_async_copy(tokens_ref, tok.at[s], local_sem.at[0]),
        pltpu.make_async_copy(
            query_ref.at[:, pl.ds(key_at, key_cols)],
            wide.at[own_rows, pl.ds(0, key_cols)],
            local_sem.at[1],
        ),
        pltpu.make_async_copy(
            key_ref.at[:, pl.ds(key_at, key_cols)],
            wide.at[own_rows, pl.ds(key_cols, key_cols)],
            local_sem.at[2],
        ),
        pltpu.make_async_copy(
            value_ref.at[:, pl.ds(value_at, value_cols)],
            wide.at[own_rows, pl.ds(2 * key_cols, value_cols)],
            local_sem.at[3],
        ),
        pltpu.make_async_copy(gate_ref, gate_all, local_sem.at[4]),
        pltpu.make_async_copy(out_weight_ref, outw.at[d], local_sem.at[5]),
    ]
    for load in loads:
        load.start()

    barrier = pltpu.get_barrier_semaphore()
    for target in (xn, yn, mate):
        pl.semaphore_signal(barrier, inc=1, device_id={"dp": target}, device_id_type=MESH)
    for offset in range(1, sp):
        pl.semaphore_signal(
            barrier, inc=1, device_id={"sp": (s + offset) % sp}, device_id_type=MESH
        )
    pl.semaphore_wait(barrier, 3 + sp - 1)

    right = (s + 1) % sp
    left = (s + sp - 1) % sp
    half = block // 2

    def tok_half(origin, number, part, target):
        ref = tok.at[origin, pl.ds(part * half, half), :]
        return push(ref, tok_send.at[number], half_recv.at[part], "sp", target)

    def token_stage(k, wait):
        if k == 0:
            tok_push(s, 0, right).start()
            tok_push(s, 1, left).start()
        if k == 1:
            tok_push(left, 0, s).wait_recv()
            tok_half(left, 2, 0, right).start()
            tok_push(right, 0, s).wait_recv()
            tok_half(right, 3, 1, left).start()
        if k == 2:
            far = (s + 2) % sp
            tok_half(far, 2, 0, s).wait_recv()
            tok_half(far, 3, 1, s).wait_recv()

    def token_drain(k):
        if k == 0:
            tok_push(s, 0, right).wait_send()
            tok_push(s, 1, left).wait_send()
        if k == 1:
            tok_half(left, 2, 0, right).wait_send()
            tok_half(right, 3, 1, left).wait_send()

    loads[0].wait()
    token_stage(0, False)
    for load in loads[1:5]:
        load.wait()
    sent = []

    def launch(copy):
        copy.start()
        sent.append(copy)

    own_gates = roles_heads // sp
    picked = lax.broadcasted_iota(jnp.int32, (own_gates, roles_heads), 0)
    wanted = picked // local_heads * head_count + s * local_heads + picked % local_heads
    chooser = jnp.where(
        lax.broadcasted_iota(jnp.int32, (own_gates, roles_heads), 1) == wanted, 1.0, 0.0
    ).astype(jnp.bfloat16)
    gates[:, pl.ds(pl.multiple_of(d * slab, slab), slab)] = jnp.dot(
        chooser, gate_all[...], preferred_element_type=jnp.float32
    ).astype(jnp.bfloat16)
    for number, target in ((0, relay_from), (1, relay_to), (2, mate)):
        launch(wide_push(d, number, target))
    for number, target in ((0, relay_from), (1, relay_to), (2, mate)):
        launch(gate_push(d, number, target))
    loads[5].wait()
    for part in range(PARTS):
        launch(outw_push(d, part, 0, relay_from))
        launch(outw_push(d, part, 2, mate))

    def await_wide(index):
        wide_push(index, 0, mate).wait_recv()
        gate_push(index, 0, mate).wait_recv()

    def await_outw(index, part):
        outw_push(index, part, 0, mate).wait_recv()

    await_wide(relay_from)
    launch(wide_push(relay_from, 3, relay_to))
    launch(gate_push(relay_from, 3, relay_to))
    launch(wide_push(relay_from, 4, mate))
    launch(gate_push(relay_from, 4, mate))
    for part in range(PARTS):
        launch(outw_push(d, part, 1, relay_to))
    await_wide(relay_to)
    launch(wide_push(relay_to, 5, mate))
    launch(gate_push(relay_to, 5, mate))
    token_stage(1, True)
    await_wide(diag)
    launch(wide_push(diag, 6, mate))
    launch(gate_push(diag, 6, mate))
    gate_pre[...] = jnp.zeros_like(gate_pre)
    for part in range(PARTS - 2):
        await_outw(relay_from, part)
        launch(outw_push(relay_from, part, 3, relay_to))
        launch(outw_push(relay_from, part, 4, mate))
    for index in (mate, xn + hop, yn + hop, diag + hop):
        await_wide(index)

    gate_lanes = 2 * roles_heads

    def project_block(index):
        flat = tok[index]
        qkv[index] = jnp.dot(flat, wide[...], preferred_element_type=jnp.float32).astype(
            jnp.bfloat16
        )
        gate_pre[index, :, :own_gates] = lax.dot_general(
            flat, gates[...], (((1,), (1,)), ((), ())), preferred_element_type=jnp.float32
        )

    def outw_relay(part):
        await_outw(relay_from, part)
        launch(outw_push(relay_from, part, 3, relay_to))
        launch(outw_push(relay_from, part, 4, mate))

    project_block(s)
    for part in range(PARTS - 2, PARTS - 1):
        outw_relay(part)
    project_block(left)
    outw_relay(PARTS - 1)
    project_block(right)
    token_stage(2, True)
    project_block((s + 2) % sp)
    projected = qkv[...].reshape(rows, qkv.shape[2])
    queries = projected[:, :key_cols]
    keys = projected[:, key_cols : 2 * key_cols]
    values = projected[:, 2 * key_cols :]
    pre = gate_pre[...].reshape(rows, gate_lanes)

    bias_parts = []
    for role in range(4):
        bias_parts.append(bias_ref[role : role + 1, :])
    bias_parts.append(jnp.zeros((1, gate_lanes - 4 * local_heads), jnp.float32))
    pre = pre + jnp.concatenate(bias_parts, axis=1)
    log_forget = jnp.minimum(pre, 0.0) - jnp.log1p(jnp.exp(-jnp.abs(pre)))
    lane = lax.broadcasted_iota(jnp.int32, pre.shape, 1)
    is_forward = lane < 2 * local_heads
    forget_sum = jnp.where(
        is_forward,
        scan_rows(log_forget, jnp.add, 0.0, False),
        scan_rows(log_forget, jnp.add, 0.0, True),
    )
    forget_sum = pltpu.roll(forget_sum, gate_lanes - local_heads, 1)
    source = pre - forget_sum
    peak = jnp.where(
        is_forward,
        scan_rows(source, jnp.maximum, -jnp.inf, False),
        scan_rows(source, jnp.maximum, -jnp.inf, True),
    )
    peak = jnp.maximum(peak, 0.0)
    floor = jnp.exp(-(forget_sum + peak))
    source_rows = jnp.transpose(source)

    row_index = lax.broadcasted_iota(jnp.int32, (rows, rows), 0)
    col_index = lax.broadcasted_iota(jnp.int32, (rows, rows), 1)
    masks = (col_index <= row_index, col_index >= row_index)
    key_lane = lax.broadcasted_iota(jnp.int32, queries.shape, 1) // key_width
    value_lane = lax.broadcasted_iota(jnp.int32, values.shape, 1) // value_width
    scale = key_width ** (-0.5)
    combined = jnp.zeros(values.shape, jnp.float32)
    for h in range(local_heads):
        head_query = jnp.where(key_lane == h, queries, jnp.zeros_like(queries))
        head_value = jnp.where(value_lane == h, values, jnp.zeros_like(values))
        raw = lax.dot_general(
            head_query, keys, (((1,), (1,)), ((), ())), preferred_element_type=jnp.float32
        )
        for direction in range(2):
            at = 2 * local_heads * direction + h
            exponent = source_rows[at : at + 1, :] - peak[:, at : at + 1]
            weights = raw * jnp.exp(jnp.where(masks[direction], exponent, -jnp.inf))
            total = jnp.sum(weights, axis=1, keepdims=True) * scale
            inverse = scale / jnp.maximum(jnp.abs(total), floor[:, at : at + 1])
            part_sum = jnp.dot(
                weights.astype(jnp.bfloat16), head_value, preferred_element_type=jnp.float32
            )
            combined = combined + part_sum * inverse
    same_head = (
        lax.broadcasted_iota(jnp.int32, (value_cols, value_cols), 0) // value_width
        == lax.broadcasted_iota(jnp.int32, (value_cols, value_cols), 1) // value_width
    )
    ones = jnp.where(same_head, 1.0, 0.0).astype(jnp.bfloat16)
    square = combined * combined
    square_high = square.astype(jnp.bfloat16)
    square_low = (square - square_high.astype(jnp.float32)).astype(jnp.bfloat16)
    mean_square = (
        jnp.dot(square_high, ones, preferred_element_type=jnp.float32)
        + jnp.dot(square_low, ones, preferred_element_type=jnp.float32)
    ) * (1.0 / value_width)
    gain = jnp.concatenate([gain_ref[h : h + 1, :] for h in range(local_heads)], axis=1)
    normed = combined * lax.rsqrt(mean_square + norm_eps) * gain
    normed_buf[...] = normed.astype(jnp.bfloat16).reshape(sp, block, value_cols)

    def norm_push(offset):
        target = (s + offset) % sp
        return pltpu.make_async_remote_copy(
            src_ref=normed_buf.at[target],
            dst_ref=hidden.at[s],
            send_sem=norm_send.at[offset - 1],
            recv_sem=norm_recv.at[offset - 1],
            device_id={"sp": target},
            device_id_type=MESH,
        )

    for offset in range(1, sp):
        launch(norm_push(offset))
    hidden[s] = normed_buf[s]

    width = outw.shape[2]

    def own_part(index):
        column = pl.ds(pl.multiple_of(index * width, width), width)
        own = pl.ds(pl.multiple_of(s * value_cols, value_cols), value_cols)
        total_out[:, column] = jnp.dot(
            hidden[s], outw[index, own, :], preferred_element_type=jnp.float32
        )

    def project(index):
        column = pl.ds(pl.multiple_of(index * width, width), width)
        total = total_out[:, column]
        for offset in range(1, sp):
            i = (s + offset) % sp
            taken = pl.ds(pl.multiple_of(i * value_cols, value_cols), value_cols)
            total = total + jnp.dot(
                hidden[i], outw[index, taken, :], preferred_element_type=jnp.float32
            )
        out_ref[:, column] = total.astype(out_ref.dtype)

    own_part(d)
    own_part(relay_from)
    for part in range(PARTS):
        await_outw(relay_to, part)
        launch(outw_push(relay_to, part, 5, mate))
    own_part(relay_to)
    for part in range(PARTS):
        await_outw(mate, part)
    own_part(mate)
    for offset in range(1, sp):
        pltpu.make_async_remote_copy(
            src_ref=normed_buf.at[s],
            dst_ref=hidden.at[(s + sp - offset) % sp],
            send_sem=norm_send.at[offset - 1],
            recv_sem=norm_recv.at[offset - 1],
            device_id={"sp": s},
            device_id_type=MESH,
        ).wait_recv()
    for part in range(PARTS):
        await_outw(diag, part)
        launch(outw_push(diag, part, 6, mate))
        if part < PARTS - 1:
            project((d, relay_from, relay_to)[part % 3])
    project(mate)
    for index in (xn + hop, yn + hop):
        for part in range(PARTS):
            await_outw(index, part)
        own_part(index)
        project(index)
    own_part(diag)
    project(diag)
    for part in range(PARTS):
        await_outw(diag + hop, part)
    own_part(diag + hop)
    project(diag + hop)
    for copy in sent:
        copy.wait_send()
    for k in range(sp):
        token_drain(k)


def fused_local(
    sp, dp, tokens, query_weight, key_weight, value_weight, gate_weight, gate_bias, norm_gain, out_weight
):
    block, width = tokens.shape[1], tokens.shape[2]
    slab, roles, head_count = gate_weight.shape
    gate_rows = jnp.transpose(gate_weight, (1, 2, 0)).reshape(roles * head_count, slab)
    value_cols = value_weight.shape[1] // sp
    wide_cols = (2 * query_weight.shape[1] + value_weight.shape[1]) // sp
    anywhere = pl.BlockSpec(memory_space=pltpu.HBM)
    vmem = pl.BlockSpec(memory_space=pltpu.VMEM)
    dma = pltpu.SemaphoreType.DMA
    bf16 = jnp.bfloat16
    output = pl.pallas_call(
        functools.partial(fused_kernel, sp, head_count),
        out_shape=jax.ShapeDtypeStruct((block, width), tokens.dtype),
        in_specs=[anywhere] * 6 + [vmem] * 2,
        out_specs=vmem,
        scratch_shapes=[
            pltpu.VMEM((sp, block, width), bf16),
            pltpu.VMEM((dp * slab, wide_cols), bf16),
            pltpu.VMEM((roles * head_count // sp, dp * slab), bf16),
            pltpu.VMEM((roles * head_count, slab), bf16),
            pltpu.VMEM((dp,) + out_weight.shape, bf16),
            pltpu.VMEM((sp, block, value_cols), bf16),
            pltpu.VMEM((sp, block, value_cols), bf16),
            pltpu.VMEM((sp, block, wide_cols), bf16),
            pltpu.VMEM((block, width), jnp.float32),
            pltpu.VMEM((sp, block, 2 * roles * head_count), jnp.float32),
            dma((6,)),
            dma((2 * sp,)),
            dma((sp,)),
            dma((2,)),
            dma((7,)),
            dma((dp,)),
            dma((7,)),
            dma((dp,)),
            dma((7, PARTS)),
            dma((dp, PARTS)),
            dma((sp - 1,)),
            dma((sp - 1,)),
        ],
        compiler_params=pltpu.CompilerParams(collective_id=0, has_side_effects=True),
    )(
        tokens[0],
        query_weight,
        key_weight,
        value_weight,
        gate_rows,
        out_weight,
        gate_bias,
        norm_gain,
    )
    return output[None]


def choose(
    sp, dp, tokens, query_weight, key_weight, value_weight, gate_weight, gate_bias, norm_gain, out_weight
):
    args = (tokens, query_weight, key_weight, value_weight, gate_weight, gate_bias, norm_gain, out_weight)
    plane_of_four_chips = dp == 2 * 2 * 2
    aligned = (
        tokens.shape[0] == 1
        and query_weight.shape[1] % (128 * sp) == 0
        and value_weight.shape[1] % (128 * sp) == 0
        and gate_weight.shape[1] * gate_weight.shape[2] == 64
    )
    if plane_of_four_chips and sp == 2 + 2 and aligned:
        return fused_local(sp, dp, *args)
    return local(*args)


def solution(mesh):
    return jax.shard_map(
        functools.partial(choose, mesh.shape["sp"], mesh.shape["dp"]),
        mesh=mesh,
        in_specs=(
            P("dp", "sp", None),
            P("dp", None),
            P("dp", None),
            P("dp", None),
            P("dp", None, None),
            P(None, "sp"),
            P("sp", None),
            P(None, "dp"),
        ),
        out_specs=P("dp", "sp", None),
        check_vma=False,
    )
```
